32 devices in a mesh: dp: 4 (over y, x), kv: 4 (over z), tp: 2 (over core).
Axes of the slice: x: 2, y: 2, z: 4, core: 2. Of those that a mesh axis runs over, the one named last changes fastest.
Arguments:
- tokens: bfloat16 [16, 4096], P('dp', ('kv', 'tp')), may hold values from -11 to 11
- attn_gain: float32 [4096], replicated, may hold values from 0.1 to 1.9
- query_weight: bfloat16 [4096, 4096], P('kv', 'tp'), may hold values from -0.09375 to 0.09375
- key_cache: bfloat16 [16, 1024, 2, 128], P('dp', 'kv', 'tp'), may hold values from -820 to 820
- value_cache: bfloat16 [16, 1024, 2, 128], P('dp', 'kv', 'tp'), may hold values from -6 to 6
- head_lambda: float32 [32], P('tp'), may hold values from 0.3 to 0.8
- head_gain: float32 [128], replicated, may hold values from 0.1 to 1.9
- out_weight: bfloat16 [4096, 4096], P('kv', 'tp'), may hold values from -0.09375 to 0.09375
- mlp_gain: float32 [4096], replicated, may hold values from 0.1 to 1.9
- gate_weight: bfloat16 [11264, 4096], P(('kv', 'tp')), may hold values from -0.09375 to 0.09375
- up_weight: bfloat16 [11264, 4096], P(('kv', 'tp')), may hold values from -0.09375 to 0.09375
- down_weight: bfloat16 [11264, 4096], P(('kv', 'tp')), may hold values from -0.078125 to 0.078125
Outputs:
- mixed: bfloat16 [16, 4096], P('dp', ('kv', 'tp'))
The draws below stay inside these ranges and needn't reach their ends.
All inputs are finite; a program needn't handle non-finite values.
Results may differ from the reference program's by a relative error of at most 0.02.
The reference program's roundings to bfloat16 on the way (of `scaled`, `rotated`, `probs`, `head_out`, `normed` and `hidden`) count: a program that leaves them out, or rounds other values in their place, can miss the bound.
Values may be sent and summed in bfloat16 or wider, within the bound.
A program may use at most 128 MiB of HBM per device.

```python
import jax
import jax.numpy as jnp
from jax import lax

D = 4096
HEADS = 32
KV_HEADS = 2
HEAD = 64
FF = 11264
VALUE = 128
GROUP = 16
BATCH = 16
CACHE_LEN = 1024
N_TP = 2


def draw_tokens(key, part):
    column_scale = 10.0 ** (jnp.arange(D, dtype=jnp.float32) / D - 0.5)
    row_scale = 10.0 ** (jax.random.uniform(jax.random.fold_in(key, 21), (BATCH, 1), jnp.float32) - 0.5)
    base = jnp.clip(jax.random.normal(jax.random.fold_in(key, 24), (BATCH, D), jnp.float32), -4.0, 4.0)
    return (0.25 * row_scale * column_scale * base).astype(jnp.bfloat16)


def draw_key_cache(key, part):
    shape = (BATCH, CACHE_LEN, KV_HEADS, 2 * HEAD)
    base = jnp.clip(jax.random.normal(jax.random.fold_in(key, 11), shape, jnp.float32), -4.0, 4.0)
    spots = jax.random.randint(jax.random.fold_in(key, 12), (BATCH, 1, KV_HEADS, 4), 0, CACHE_LEN - 1)
    strength = jax.random.uniform(jax.random.fold_in(key, 13), (BATCH, 1, KV_HEADS, 4), jnp.float32, 100.0, 200.0)
    flips = jax.random.randint(jax.random.fold_in(key, 14), (BATCH, 1, KV_HEADS, 4), 0, 2)
    signed = strength * (2.0 * flips.astype(jnp.float32) - 1.0)
    place = jnp.arange(CACHE_LEN, dtype=jnp.int32).reshape(1, CACHE_LEN, 1, 1)
    hits = place == spots
    factor = jnp.sum(jnp.where(hits, signed, 0.0), axis=-1, keepdims=True)
    marked = jnp.any(hits, axis=-1, keepdims=True)
    follow_factor = jnp.roll(factor, 1, axis=1)
    follow = jnp.logical_and(jnp.roll(marked, 1, axis=1), jnp.logical_not(marked))
    lifted = jnp.roll(base, 1, axis=1)
    planted = jnp.where(marked, factor * base, jnp.where(follow, 1.01 * follow_factor * lifted, 2.0 * base))
    return planted.astype(jnp.bfloat16)


def spiked(array, stream_key, source, target, blocks, factor):
    def block_of(dim):
        return (jnp.arange(array.shape[dim]) // (array.shape[dim] // blocks)).reshape((-1,) + (1,) * (array.ndim - 1 - dim))

    one_side = jax.random.permutation(stream_key, blocks)[block_of(target)]
    second = (block_of(target) + blocks // 2) % blocks
    return jnp.where((block_of(source) == one_side) | (block_of(source) == second), factor * array, array)


def levels(stream_key, dims, split, least, high):
    loudness, own = 1.0, jax.random.fold_in(stream_key, 6)
    for axis_at, blocks in split:
        steps = jnp.exp(jax.random.uniform(jax.random.fold_in(own, axis_at), (blocks,), jnp.float32, least / len(split), high / len(split)))
        loudness = loudness * jnp.repeat(steps, dims[axis_at] // blocks).reshape([-1 if axis == axis_at else 1 for axis in range(len(dims))])
    return loudness


def gaussian(own_key, dims, scale, most, cuts=(), kind=jnp.bfloat16):
    result = scale * jax.random.normal(own_key, dims, jnp.float32)
    if cuts:
        result = result * levels(own_key, dims, cuts, -0.22, 0.18)
    return jnp.clip(result, -most, most).astype(kind)


def gaussian_with(stream_key, dims, deviation, limit, pieces, heavy, kind=jnp.bfloat16):
    values = deviation * jax.random.normal(stream_key, dims, jnp.float32)
    if pieces:
        values = values * levels(stream_key, dims, pieces, -0.22, 0.18)
    return jnp.clip(spiked(values, jax.random.fold_in(stream_key, 3), *heavy), -limit, limit).astype(kind)


def setup_inputs(seed: int = 0) -> dict:
    key_of = jax.random.split(jax.random.key(seed), 13)
    return {
        "tokens": draw_tokens(jax.random.fold_in(key_of[12], 71), 0),
        "attn_gain": jnp.clip(1.0 + 0.18 * jax.random.normal(key_of[1], (D,), jnp.float32), 0.1, 1.9),
        "query_weight": gaussian(key_of[2], (D, HEADS * 2 * HEAD), D ** -0.5, 0.09375, ((0, 4), (1, 2))),
        "key_cache": draw_key_cache(jax.random.fold_in(key_of[12], 71), 0),
        "value_cache": gaussian(key_of[4], (BATCH, CACHE_LEN, KV_HEADS, VALUE), 1.0, 6.0, ((0, 4), (1, 4), (2, 2))),
        "head_lambda": jnp.clip(0.3 + 0.5 * jax.random.uniform(key_of[5], (HEADS,), jnp.float32) ** levels(key_of[5], (HEADS,), ((0, 2),), -0.2, 0.2), 0.3, 0.8),
        "head_gain": jnp.clip(1.0 + 0.18 * jax.random.normal(key_of[6], (VALUE,), jnp.float32), 0.1, 1.9),
        "out_weight": gaussian(key_of[7], (D, HEADS * VALUE), (HEADS * VALUE) ** -0.5, 0.09375, ((0, 4), (1, 2))),
        "mlp_gain": jnp.clip(1.0 + 0.18 * jax.random.normal(key_of[8], (D,), jnp.float32), 0.1, 1.9),
        "gate_weight": gaussian(key_of[9], (FF, D), D ** -0.5, 0.09375, ((0, 8),)),
        "up_weight": gaussian(key_of[10], (FF, D), D ** -0.5, 0.09375, ((0, 8),)),
        "down_weight": gaussian_with(key_of[11], (FF, D), FF ** -0.5, 0.078125, ((0, 8),), (0, 1, 8, 2.0)),
    }


EPS = 1e-06
THETA = 10000.0

def rotate(vector, position):
    half_len = vector.shape[-1] // 2
    inv_freq = 1.0 / THETA ** (jnp.arange(half_len, dtype=jnp.float32) / half_len)
    angles = position * inv_freq
    cos_table = jnp.cos(angles)
    sin_table = jnp.sin(angles)
    first_half = vector[..., :half_len]
    second_half = vector[..., half_len:]
    return jnp.concatenate([first_half * cos_table - second_half * sin_table, second_half * cos_table + first_half * sin_table], axis=-1)

def reference(tokens, attn_gain, query_weight, key_cache, value_cache, head_lambda, head_gain, out_weight, mlp_gain, gate_weight, up_weight, down_weight):
    as_float = tokens.astype(jnp.float32)
    mean_square = lax.optimization_barrier(jnp.mean(as_float * as_float, axis=-1, keepdims=True))
    scaled = (as_float * attn_gain).astype(jnp.bfloat16)
    queries = jnp.dot(scaled, query_weight, preferred_element_type=jnp.float32) * lax.rsqrt(mean_square + EPS)
    queries = queries.reshape(BATCH, HEADS, 2, HEAD)
    rotated = rotate(queries, jnp.float32(CACHE_LEN)).astype(jnp.bfloat16)
    lam_grid = head_lambda.reshape(KV_HEADS, GROUP, 1)

    def attend(item):
        query_row, key_rows, value_rows = item
        query_grid = query_row.reshape(KV_HEADS, GROUP, 2, HEAD).astype(jnp.float32)
        key_grid = key_rows.reshape(CACHE_LEN, KV_HEADS, 2, HEAD).astype(jnp.float32)
        scores = jnp.einsum('kgch,lkch->kgcl', query_grid, key_grid) * HEAD ** (-0.5)
        top_score = lax.optimization_barrier(jnp.max(scores, axis=-1, keepdims=True))
        weights_exp = jnp.exp(scores - top_score)
        exp_total = lax.optimization_barrier(jnp.sum(weights_exp, axis=-1))
        probs = weights_exp.astype(jnp.bfloat16).astype(jnp.float32)
        weighted = jnp.einsum('kgcl,lkv->kgcv', probs, value_rows.astype(jnp.float32))
        attended = weighted / exp_total[..., None]
        difference = attended[:, :, 0] - lam_grid * attended[:, :, 1]
        head_norm = lax.rsqrt(lax.optimization_barrier(jnp.mean(difference * difference, axis=-1, keepdims=True)) + EPS)
        head_out = difference * head_norm * head_gain
        return head_out.reshape(HEADS * VALUE).astype(jnp.bfloat16)
    head_out = lax.map(attend, (rotated, key_cache, value_cache))
    group_rows = HEADS * VALUE // N_TP
    attention = jnp.zeros((BATCH, D), jnp.float32)
    for tp_slot in range(N_TP):
        block_out = lax.dot_general(head_out[:, tp_slot * group_rows:(tp_slot + 1) * group_rows], out_weight[:, tp_slot * group_rows:(tp_slot + 1) * group_rows], (((1,), (1,)), ((), ())), preferred_element_type=jnp.float32).astype(jnp.bfloat16)
        attention = attention + block_out.astype(jnp.float32)
    stream = as_float + attention
    stream_square = lax.optimization_barrier(jnp.mean(stream * stream, axis=-1, keepdims=True))
    normed = (stream * lax.rsqrt(stream_square + EPS) * mlp_gain).astype(jnp.bfloat16)
    gate_out = lax.dot_general(normed, gate_weight, (((1,), (1,)), ((), ())), preferred_element_type=jnp.float32)
    up_out = lax.dot_general(normed, up_weight, (((1,), (1,)), ((), ())), preferred_element_type=jnp.float32)
    hidden = (jax.nn.silu(gate_out) * up_out).astype(jnp.bfloat16)
    down_out = jnp.dot(hidden, down_weight, preferred_element_type=jnp.float32)
    return (stream + down_out).astype(jnp.bfloat16)
```

```python
import functools

import jax
import jax.numpy as jnp
import numpy as np
from jax import lax
from jax.experimental import pallas as pl
from jax.experimental.pallas import tpu as pltpu
from jax.sharding import PartitionSpec as P

EPS = 1e-06
THETA = 10000.0
LANES = 128
CUTS = (10, 19, 22)
AHEAD = 8


def merged(x, axis, combine):
    everything = jax.tree.map(lambda part: lax.all_gather(part, axis), x)
    first = jax.tree.map(lambda part: part[0], everything)

    def hop(k, so_far):
        return combine(so_far, jax.tree.map(lambda part: part[k], everything))

    return lax.fori_loop(1, lax.axis_size(axis), hop, first)


def rotate(vector, position):
    half_len = vector.shape[-1] // 2
    inv_freq = 1.0 / THETA ** (jnp.arange(half_len, dtype=jnp.float32) / half_len)
    angles = position * inv_freq
    cos_table = jnp.cos(angles)
    sin_table = jnp.sin(angles)
    first_half = vector[..., :half_len]
    second_half = vector[..., half_len:]
    return jnp.concatenate(
        [
            first_half * cos_table - second_half * sin_table,
            second_half * cos_table + first_half * sin_table,
        ],
        axis=-1,
    )


def combine(earlier, latter):
    peak_a, total_a, value_a = earlier
    peak_b, total_b, value_b = latter
    peak_new = jnp.maximum(peak_a, peak_b)
    factor_a = jnp.exp(peak_a - peak_new)
    factor_b = jnp.exp(peak_b - peak_new)
    return (
        peak_new,
        total_a * factor_a + total_b * factor_b,
        value_a * factor_a[..., None] + value_b * factor_b[..., None],
    )


def inner_last(left, right):
    return lax.dot_general(
        left, right, (((1,), (1,)), ((), ())), preferred_element_type=jnp.float32
    )


def shards(
    tokens,
    attn_gain,
    query_weight,
    key_cache,
    value_cache,
    head_lambda,
    head_gain,
    out_weight,
    mlp_gain,
    gate_weight,
    up_weight,
    down_weight,
):
    row_count = tokens.shape[0]
    kv_count = lax.axis_size("kv")
    tp_count = lax.axis_size("tp")
    kv_index = lax.axis_index("kv")
    row_span = query_weight.shape[0]
    full_rows = lax.all_gather(tokens, ("kv", "tp"), axis=1, tiled=True)
    wide_rows = full_rows.astype(jnp.float32)
    mean_square = jnp.mean(wide_rows * wide_rows, axis=-1, keepdims=True)
    scaled = (wide_rows * attn_gain).astype(jnp.bfloat16)
    local_cols = lax.dynamic_slice_in_dim(scaled, kv_index * row_span, row_span, 1)
    queries = lax.psum(jnp.dot(local_cols, query_weight, preferred_element_type=jnp.float32), "kv")
    queries = queries * lax.rsqrt(mean_square + EPS)
    head_count = head_lambda.shape[0]
    kv_local = key_cache.shape[2]
    group_size = head_count // kv_local
    position_count = key_cache.shape[1]
    half_dim = key_cache.shape[3] // 2
    value_dim = value_cache.shape[3]
    queries = queries.reshape(row_count, kv_local, group_size, 2, half_dim)
    rotated = rotate(queries, jnp.float32(position_count * kv_count)).astype(jnp.bfloat16)
    key_grid = key_cache.reshape(row_count, position_count, kv_local, 2, half_dim)
    scores = jnp.einsum(
        "bkgch,bpkch->bkgcp", rotated, key_grid, preferred_element_type=jnp.float32
    ) * half_dim ** (-0.5)
    local_peak = jnp.max(scores, axis=-1)
    weights_exp = jnp.exp(scores - local_peak[..., None])
    lam_grid = head_lambda.reshape(kv_local, group_size)[None, :, :, None]
    exp_total = jnp.sum(weights_exp, axis=-1)
    weighted = jnp.einsum(
        "bkgcp,bpkv->bkgcv",
        weights_exp.astype(jnp.bfloat16),
        value_cache,
        preferred_element_type=jnp.float32,
    )
    peak_all, total_all, weighted_all = merged((local_peak, exp_total, weighted), "kv", combine)
    attended = weighted_all / total_all[..., None]
    difference = attended[:, :, :, 0] - lam_grid * attended[:, :, :, 1]
    head_norm = lax.rsqrt(jnp.mean(difference * difference, axis=-1, keepdims=True) + EPS)
    head_out = (difference * head_norm * head_gain).reshape(row_count, head_count * value_dim)
    head_out = head_out.astype(jnp.bfloat16)
    out_part = inner_last(head_out, out_weight).astype(jnp.bfloat16)
    pieces = lax.all_gather(out_part, ("kv", "tp"), axis=1, tiled=True)
    attention = jnp.sum(
        pieces.astype(jnp.float32).reshape(row_count, kv_count, tp_count, -1), axis=2
    )
    stream = wide_rows + attention.reshape(row_count, -1)
    stream_square = jnp.mean(stream * stream, axis=-1, keepdims=True)
    normed = (stream * lax.rsqrt(stream_square + EPS) * mlp_gain).astype(jnp.bfloat16)
    gate_out = inner_last(normed, gate_weight)
    up_out = inner_last(normed, up_weight)
    hidden = (jax.nn.silu(gate_out) * up_out).astype(jnp.bfloat16)
    own_cols = tokens.shape[1]
    down_cols = lax.psum_scatter(
        lax.dot_general(
            down_weight, hidden, (((0,), (1,)), ((), ())), preferred_element_type=jnp.float32
        ),
        ("kv", "tp"),
        scatter_dimension=0,
        tiled=True,
    )
    column_index = lax.axis_index(("kv", "tp"))
    own_stream = lax.dynamic_slice_in_dim(stream, column_index * own_cols, own_cols, 1)
    return (own_stream + down_cols.T).astype(jnp.bfloat16)


def fused_kernel(
    kv_n, tp_n, tok_h, again_h, wq_h, kc_h, vc_h, lam_h, hgain_h, wo_h, mgain_h, wg_h, wu_h, wd_h,
    table_h,
    out,
    again, lam, hgain, mgain, table,
    wq, kc, vc, wo, stage, wgu_t, wd,
    tg, qa, qf, ms, mb, mv, st, cf, hf, og, stream, ga, hid, ds, dr,
    hand, lsem, wqsem, wsem, csem,
    tsend, trecv, qsend, qrecv, ssend, srecv, msend, mrecv, osend, orecv, dsend, drecv,
):
    kv, tp = lax.axis_index("kv"), lax.axis_index("tp")
    n_all = kv_n * tp_n
    me = kv * tp_n + tp
    rows, own = tg.shape[1:]
    mate = {"kv": kv, "tp": lax.rem(tp + 1, tp_n)}
    heads, value_dim = hf.shape[1], hf.shape[2]
    both = 2 * heads
    features = wo.shape[0]
    units = wd.shape[0]
    per_weight = units // LANES
    chunks = 2 * per_weight
    slots = stage.shape[0]
    per = 4
    pieces = heads // per
    width = per * value_dim

    def query_load(j):
        cols = pl.ds(j * width, width)
        return pltpu.make_async_copy(wq_h.at[:, cols], wq.at[:, cols], wqsem.at[j])

    token_load = pltpu.make_async_copy(tok_h, tg.at[me], lsem.at[0])
    token_load.start()
    for j in range(pieces):
        query_load(j).start()
    small_loads = [
        pltpu.make_async_copy(source, target, lsem.at[slot + 1])
        for slot, (source, target) in enumerate(
            [(again_h, again), (table_h, table), (lam_h, lam), (hgain_h, hgain), (mgain_h, mgain)]
        )
    ]
    for load in small_loads:
        load.start()

    def chunk_load(weight, i, slot):
        piece = pl.ds(pl.multiple_of(i * LANES, LANES), LANES)
        at = i if weight is wg_h else i + per_weight
        return pltpu.make_async_copy(weight.at[piece], stage.at[slot], csem.at[at])

    def later_load(i):
        @pl.when(i < per_weight)
        def _():
            chunk_load(wg_h, i, lax.rem(i, slots)).start()

        @pl.when((i >= per_weight) & (i < chunks))
        def _():
            chunk_load(wu_h, i - per_weight, lax.rem(i, slots)).start()

    def turn(low, high):
        def turn_gate(i, carry):
            slot = lax.rem(i, slots)
            later_load(i + AHEAD)
            chunk_load(wg_h, i, slot).wait()
            at = pl.ds(pl.multiple_of(i * LANES, LANES), LANES)
            wgu_t[0, :, at] = stage[slot].T
            return carry

        def turn_up(i, carry):
            slot = lax.rem(i + per_weight, slots)
            later_load(i + per_weight + AHEAD)
            chunk_load(wu_h, i, slot).wait()
            at = pl.ds(pl.multiple_of(i * LANES, LANES), LANES)
            wgu_t[1, :, at] = stage[slot].T
            return carry

        low, high = chunks * low // 22, chunks * high // 22
        if low < per_weight:
            lax.fori_loop(low, min(high, per_weight), turn_gate, 0)
        if high > per_weight:
            lax.fori_loop(max(low, per_weight) - per_weight, high - per_weight, turn_up, 0)

    half_way = kv_n // 2

    def far(i):
        down = kv_n - 1 - i
        down = down - 1 + lax.div(down - kv + kv_n - 1, kv_n)
        up = i + 1 - lax.div(kv - i + kv_n - 1, kv_n)
        low = 1 - lax.div(kv, half_way)
        return up + low * (down - up)

    others = [far(i) for i in range(kv_n - 1)]

    def remote(src, dst, send, recv, where):
        copy = pltpu.make_async_remote_copy(
            src_ref=src, dst_ref=dst, send_sem=send, recv_sem=recv,
            device_id=where, device_id_type=pl.DeviceIdType.MESH,
        )
        copy.start()
        return copy

    def arrived(dst, recv):
        pltpu.make_async_remote_copy(
            src_ref=dst, dst_ref=dst, send_sem=recv, recv_sem=recv,
            device_id=mate, device_id_type=pl.DeviceIdType.MESH,
        ).wait_recv()

    def signal(semaphore, where):
        pl.semaphore_signal(
            semaphore, inc=1, device_id=where, device_id_type=pl.DeviceIdType.MESH
        )

    barrier = pltpu.get_barrier_semaphore()
    for z in others:
        signal(barrier, {"kv": z, "tp": tp_n - 1})

    @pl.when(tp == tp_n - 1)
    def _():
        signal(barrier, mate)

    @pl.when(tp == 0)
    def _():
        pl.semaphore_wait(barrier, 1)
        signal(hand.at[0], mate)

    @pl.when(tp == tp_n - 1)
    def _():
        pl.semaphore_wait(hand.at[0], 1)

    sends = []
    token_load.wait()
    sends.append(remote(tg.at[me], tg.at[me], tsend.at[0], trecv.at[me], mate))
    small_loads[0].wait()
    at_mate = kv * tp_n + lax.rem(tp + 1, tp_n)
    arrived(tg.at[at_mate], trecv.at[at_mate])
    parts = []
    square = jnp.zeros((rows, 1), jnp.float32)
    for side in range(tp_n):
        at = kv * tp_n + side
        gain = again[:, pl.ds(pl.multiple_of(at * own, LANES), own)]
        wide = tg[at].astype(jnp.float32)
        square = square + jnp.sum(wide * wide, axis=1, keepdims=True)
        parts.append((wide * gain).astype(jnp.bfloat16))
    scaled = jnp.concatenate(parts, axis=1)
    qa[kv, heads] = jnp.broadcast_to(square, (rows, value_dim))

    def query_piece(j):
        query_load(j).wait()
        product = jnp.dot(
            scaled, wq[:, j * width:(j + 1) * width], preferred_element_type=jnp.float32
        )
        for i in range(per):
            qa[kv, j * per + i] = product[:, i * value_dim:(i + 1) * value_dim]

    def query_part(j):
        return pl.ds(j * per, per + (1 if j == pieces - 1 else 0))

    key_load = pltpu.make_async_copy(kc_h, kc, wsem.at[0])
    value_load = pltpu.make_async_copy(vc_h, vc, wsem.at[1])
    out_load = pltpu.make_async_copy(wo_h, wo, wsem.at[2])
    down_load = pltpu.make_async_copy(wd_h, wd, wsem.at[3])

    for j in range(pieces):
        query_piece(j)
        if j == 0:
            key_load.start()
            value_load.start()
            for i in range(AHEAD):
                if i < per_weight:
                    chunk_load(wg_h, i, i % slots).start()
                elif i < chunks:
                    chunk_load(wu_h, i - per_weight, i % slots).start()

            @pl.when(tp == tp_n - 1)
            def _():
                pl.semaphore_wait(barrier, tp_n * (kv_n - 1))
                signal(hand.at[1], mate)

            @pl.when(tp == 0)
            def _():
                pl.semaphore_wait(hand.at[1], 1)

        part = query_part(j)
        for i, z in enumerate(others):
            sends.append(
                remote(
                    qa.at[kv, part], qa.at[kv, part],
                    qsend.at[j, i], qrecv.at[j, kv], {"kv": z, "tp": tp},
                )
            )

    slot = 1
    for z in others:
        for side in range(tp_n):
            sends.append(
                remote(
                    tg.at[me], tg.at[me], tsend.at[slot], trecv.at[me], {"kv": z, "tp": side}
                )
            )
            slot += 1

    turn(0, CUTS[0])
    out_load.start()
    for load in small_loads[1:]:
        load.wait()
    for z in others[::-1]:
        for j in range(pieces):
            arrived(qa.at[z, query_part(j)], qrecv.at[j, z])
    square = qa[0, heads]
    for z in range(1, kv_n):
        square = square + qa[z, heads]
    scale = lax.rsqrt(square / (n_all * own) + EPS)
    lane = lax.broadcasted_iota(jnp.int32, (rows, value_dim), 1)
    half = value_dim // 2
    first = lax.rem(lane, half) < half // 2
    cosines = table[0:1, :]
    sines = table[1:2, :]
    for h in range(heads):
        total = qa[0, h]
        for z in range(1, kv_n):
            total = total + qa[z, h]
        total = total * scale
        swapped = jnp.where(
            first,
            pltpu.roll(total, value_dim - half // 2, 1),
            pltpu.roll(total, half // 2, 1),
        )
        qf[h] = total * cosines + swapped * sines

    key_load.wait()
    value_load.wait()
    low = lax.broadcasted_iota(jnp.int32, (heads, value_dim), 1) < half
    row_at = lax.broadcasted_iota(jnp.int32, (both, value_dim), 0)
    lane_at = lax.broadcasted_iota(jnp.int32, (both, value_dim), 1)
    spread = []
    for b in range(rows):
        query = qf[:, b, :]
        grid = jnp.concatenate(
            [jnp.where(low, query, 0.0), jnp.where(low, 0.0, query)], axis=0
        ).astype(jnp.bfloat16)
        scores = inner_last(grid, kc[b]) * half ** (-0.5)
        peak = jnp.max(scores, axis=1, keepdims=True)
        exps = jnp.exp(scores - peak)
        sums = jnp.sum(exps, axis=1, keepdims=True)
        spread.append(exps.astype(jnp.bfloat16))
        stats = jnp.where(lane_at == row_at, peak, 0.0) + jnp.where(
            lane_at == row_at + both, sums, 0.0
        )
        st[kv, b:b + 1, :] = jnp.sum(stats, axis=0, keepdims=True)
    for i, z in enumerate(others):
        sends.append(
            remote(
                st.at[kv], st.at[kv], ssend.at[i], srecv.at[kv], {"kv": z, "tp": tp}
            )
        )
    for b in range(rows):
        values = jnp.dot(spread[b], vc[b], preferred_element_type=jnp.float32)
        ms[b] = values
        mb[b] = values.astype(jnp.bfloat16)
    for b in range(rows):
        for i, z in enumerate(others):
            sends.append(
                remote(
                    mb.at[b], mv.at[kv, b],
                    msend.at[b, i], mrecv.at[b, kv], {"kv": z, "tp": tp},
                )
            )

    down_load.start()
    turn(CUTS[0], CUTS[1])
    lam_at = lax.broadcasted_iota(jnp.int32, (heads, heads), 0)
    lam_lane = lax.broadcasted_iota(jnp.int32, (heads, heads), 1)
    lam_col = jnp.sum(
        jnp.where(lam_at == lam_lane, lam[...], 0.0), axis=1, keepdims=True
    )
    signs = jnp.concatenate([jnp.ones((heads, 1), jnp.float32), -lam_col], axis=0)
    sources = [kv] + others[::-1]
    for z in sources[1:]:
        arrived(st.at[z], srecv.at[z])
    for b in range(rows):
        peaks, sums = [], []
        for z in sources:
            stats = st[z, b:b + 1, :]
            peaks.append(
                jnp.sum(jnp.where(lane_at == row_at, stats, 0.0), axis=1, keepdims=True)
            )
            sums.append(
                jnp.sum(jnp.where(lane_at == row_at + both, stats, 0.0), axis=1, keepdims=True)
            )
        top = peaks[0]
        for peak in peaks[1:]:
            top = jnp.maximum(top, peak)
        factors = [jnp.exp(peak - top) for peak in peaks]
        all_sums = jnp.zeros_like(top)
        for factor, total in zip(factors, sums):
            all_sums = all_sums + total * factor
        share = signs / all_sums
        for at, factor in enumerate(factors):
            cf[at, b] = jnp.broadcast_to(factor * share, (both, value_dim))
    for b in range(rows):
        for z in sources[1:]:
            arrived(mv.at[z, b], mrecv.at[b, z])
    for b in range(rows):
        weighted = ms[b] * cf[0, b]
        for at, z in enumerate(sources[1:]):
            weighted = weighted + mv[z, b].astype(jnp.float32) * cf[at + 1, b]
        difference = weighted[0:heads] + weighted[heads:both]
        norm = lax.rsqrt(jnp.mean(difference * difference, axis=1, keepdims=True) + EPS)
        hf[b] = difference * norm * hgain[...]
    flat = jnp.concatenate(
        [hf[:, h, :] for h in range(heads)], axis=1
    ).astype(jnp.bfloat16)
    out_load.wait()
    cut = features // 2
    for j in range(2):
        cols = pl.ds(j * cut, cut)
        og[me, :, cols] = inner_last(flat, wo[j * cut:(j + 1) * cut, :]).astype(jnp.bfloat16)
        slot = 0
        for z in others:
            for side in range(tp_n):
                sends.append(
                    remote(
                        og.at[me, :, cols], og.at[me, :, cols],
                        osend.at[j, slot], orecv.at[j, me], {"kv": z, "tp": side},
                    )
                )
                slot += 1
        sends.append(
            remote(
                og.at[me, :, cols], og.at[me, :, cols], osend.at[j, slot], orecv.at[j, me], mate
            )
        )

    turn(CUTS[1], CUTS[2])
    for z in others:
        for side in range(tp_n):
            at = z * tp_n + side
            arrived(tg.at[at], trecv.at[at])
    square = jnp.zeros((rows, 1), jnp.float32)
    for order, z in enumerate(sources):
        for side in range(tp_n):
            at = z * tp_n + side
            for j in range(2):
                cols = pl.ds(j * cut, cut)
                if order == 0:
                    continue
                arrived(og.at[at, :, cols], orecv.at[j, at])
        if order == 0:
            for j in range(2):
                cols = pl.ds(j * cut, cut)
                arrived(og.at[at_mate, :, cols], orecv.at[j, at_mate])
        tokens = jnp.concatenate(
            [tg[z * tp_n + side].astype(jnp.float32) for side in range(tp_n)], axis=1
        )
        attention = og[z * tp_n].astype(jnp.float32)
        for side in range(1, tp_n):
            attention = attention + og[z * tp_n + side].astype(jnp.float32)
        piece = tokens + attention
        at = pl.ds(pl.multiple_of(z * features, LANES), features)
        stream[:, at] = piece
        square = square + jnp.sum(piece * piece, axis=1, keepdims=True)
        gained = (piece * mgain[:, at]).astype(jnp.bfloat16)
        for g in range(2):
            product = jnp.dot(gained, wgu_t[g, at, :], preferred_element_type=jnp.float32)
            if order == 0:
                ga[g] = product
            else:
                ga[g] = ga[g] + product
    scale = lax.rsqrt(square / (n_all * own) + EPS)
    gate = ga[0] * scale
    up = ga[1] * scale
    hid[...] = (gate / (1.0 + jnp.exp(-gate)) * up).astype(jnp.bfloat16)
    hidden = hid[...]
    down_load.wait()

    def down_block(at):
        return jnp.dot(
            hidden,
            wd[:, pl.ds(pl.multiple_of(at * own, LANES), own)],
            preferred_element_type=jnp.float32,
        )

    targets = []
    for z in others:
        for side in range(tp_n):
            targets.append((z * tp_n + side, {"kv": z, "tp": side}))
    targets.append((at_mate, mate))
    pending = None

    def down_send(slot, block):
        at, where = targets[slot]
        ds[at] = block.astype(ds.dtype)
        sends.append(
            remote(ds.at[at], dr.at[me], dsend.at[slot], drecv.at[me], where)
        )

    for slot, (at, _) in enumerate(targets):
        block = down_block(at)
        if pending is not None:
            down_send(slot - 1, pending)
        pending = block
    total = down_block(me)
    down_send(len(targets) - 1, pending)
    total = total + stream[:, pl.ds(pl.multiple_of(me * own, LANES), own)]
    arrived(dr.at[at_mate], drecv.at[at_mate])
    total = total + dr[at_mate].astype(jnp.float32)
    for z in others[::-1]:
        for side in range(tp_n):
            at = z * tp_n + side
            arrived(dr.at[at], drecv.at[at])
    for z in others[::-1]:
        for side in range(tp_n):
            total = total + dr[z * tp_n + side].astype(jnp.float32)
    out[...] = total.astype(out.dtype)
    for copy in sends:
        copy.wait_send()


def turning(head_dim, position):
    half_len = head_dim // 4
    inv_freq = np.float32(1.0) / np.float32(THETA) ** (
        np.arange(half_len, dtype=np.float32) / np.float32(half_len)
    )
    angles = (np.float32(position) * inv_freq.astype(np.float32)).astype(np.float32)
    cos, sin = np.cos(angles), np.sin(angles)
    return np.stack(
        [np.concatenate([cos, cos] * 2), np.concatenate([-sin, sin] * 2)]
    ).astype(np.float32)


def fused(kv_n, tp_n, *arrays):
    (tokens, attn_gain, wq, kc, vc, lam, hgain, wo, mgain, wg, wu, wd) = arrays
    rows, own = tokens.shape
    n_all = kv_n * tp_n
    positions, value_dim = kc.shape[1], kc.shape[3]
    heads = lam.shape[0]
    both = 2 * heads
    model = n_all * own
    per_weight = wg.shape[0] // LANES
    pieces = heads // 4
    f32, bf16 = jnp.float32, jnp.bfloat16
    table = jnp.asarray(turning(value_dim, positions * kv_n))
    dma = pltpu.SemaphoreType.DMA
    hbm = pl.BlockSpec(memory_space=pl.ANY)
    return pl.pallas_call(
        functools.partial(fused_kernel, kv_n, tp_n),
        out_shape=pltpu.VMEM((rows, own), tokens.dtype),
        in_specs=[hbm] * 13,
        out_specs=pl.BlockSpec(memory_space=pltpu.VMEM),
        scratch_shapes=[
            pltpu.VMEM((1, model), f32),
            pltpu.VMEM((1, heads), f32),
            pltpu.VMEM((1, value_dim), f32),
            pltpu.VMEM((1, model), f32),
            pltpu.VMEM((2, value_dim), f32),
            pltpu.VMEM(wq.shape, bf16),
            pltpu.VMEM((rows, positions, value_dim), bf16),
            pltpu.VMEM((rows, positions, value_dim), bf16),
            pltpu.VMEM(wo.shape, bf16),
            pltpu.VMEM((min(AHEAD + 1, 2 * per_weight), LANES, model), bf16),
            pltpu.VMEM((2,) + wg.shape[::-1], bf16),
            pltpu.VMEM(wd.shape, bf16),
            pltpu.VMEM((n_all, rows, own), bf16),
            pltpu.VMEM((kv_n, heads + 1, rows, value_dim), f32),
            pltpu.VMEM((heads, rows, value_dim), f32),
            pltpu.VMEM((rows, both, value_dim), f32),
            pltpu.VMEM((rows, both, value_dim), bf16),
            pltpu.VMEM((kv_n, rows, both, value_dim), bf16),
            pltpu.VMEM((kv_n, rows, value_dim), f32),
            pltpu.VMEM((kv_n, rows, both, value_dim), f32),
            pltpu.VMEM((rows, heads, value_dim), f32),
            pltpu.VMEM((n_all, rows, wo.shape[0]), bf16),
            pltpu.VMEM((rows, model), f32),
            pltpu.VMEM((2, rows, wg.shape[0]), f32),
            pltpu.VMEM((rows, wg.shape[0]), bf16),
            pltpu.VMEM((n_all, rows, own), bf16),
            pltpu.VMEM((n_all, rows, own), bf16),
            pltpu.SemaphoreType.REGULAR((2,)),
            dma((6,)), dma((pieces,)), dma((4,)), dma((2 * per_weight,)),
            dma((n_all,)), dma((n_all,)),
            dma((pieces, kv_n - 1)), dma((pieces, kv_n)),
            dma((kv_n - 1,)), dma((kv_n,)),
            dma((rows, kv_n - 1)), dma((rows, kv_n)),
            dma((2, n_all - 1)), dma((2, n_all)),
            dma((n_all - 1,)), dma((n_all,)),
        ],
        compiler_params=pltpu.CompilerParams(
            collective_id=0, has_side_effects=True, vmem_limit_bytes=65000000
        ),
    )(
        tokens, attn_gain.reshape(1, -1), wq,
        kc.reshape(rows, positions, value_dim), vc.reshape(rows, positions, value_dim),
        lam.reshape(1, -1), hgain.reshape(1, -1), wo, mgain.reshape(1, -1), wg, wu, wd, table,
    )


def layer(kv_n, tp_n, *arrays):
    tokens, kc, wg = arrays[0], arrays[3], arrays[9]
    small = tokens.shape[0] == kv_n and kc.shape[2] == 1 and tp_n == 2
    if small and tokens.shape[1] % LANES == 0 and wg.shape[0] % LANES == 0:
        return fused(kv_n, tp_n, *arrays)
    return shards(*arrays)


def solution(mesh):
    placed = (
        P("dp", ("kv", "tp")),
        P(),
        P("kv", "tp"),
        P("dp", "kv", "tp", None),
        P("dp", "kv", "tp", None),
        P("tp"),
        P(),
        P("kv", "tp"),
        P(),
        P(("kv", "tp"), None),
        P(("kv", "tp"), None),
        P(("kv", "tp"), None),
    )
    return jax.shard_map(
        functools.partial(layer, mesh.shape["kv"], mesh.shape["tp"]),
        mesh=mesh, in_specs=placed, out_specs=P("dp", ("kv", "tp")), check_vma=False
    )
```

```python
import functools

import jax
import jax.numpy as jnp
import numpy as np
from jax import lax
from jax.experimental import pallas as pl
from jax.experimental.pallas import tpu as pltpu
from jax.sharding import PartitionSpec as P

EPS = 1e-06
THETA = 10000.0
LANES = 128
AHEAD = 8
MARKS = (0, 4, 8, 9, 10, 14, 15, 17, 22)


def merged(x, axis, combine):
    everything = jax.tree.map(lambda part: lax.all_gather(part, axis), x)
    first = jax.tree.map(lambda part: part[0], everything)

    def hop(k, so_far):
        return combine(so_far, jax.tree.map(lambda part: part[k], everything))

    return lax.fori_loop(1, lax.axis_size(axis), hop, first)


def rotate(vector, position):
    half_len = vector.shape[-1] // 2
    inv_freq = 1.0 / THETA ** (jnp.arange(half_len, dtype=jnp.float32) / half_len)
    angles = position * inv_freq
    cos_table = jnp.cos(angles)
    sin_table = jnp.sin(angles)
    first_half = vector[..., :half_len]
    second_half = vector[..., half_len:]
    return jnp.concatenate(
        [
            first_half * cos_table - second_half * sin_table,
            second_half * cos_table + first_half * sin_table,
        ],
        axis=-1,
    )


def combine(earlier, latter):
    peak_a, total_a, value_a = earlier
    peak_b, total_b, value_b = latter
    peak_new = jnp.maximum(peak_a, peak_b)
    factor_a = jnp.exp(peak_a - peak_new)
    factor_b = jnp.exp(peak_b - peak_new)
    return (
        peak_new,
        total_a * factor_a + total_b * factor_b,
        value_a * factor_a[..., None] + value_b * factor_b[..., None],
    )


def inner_last(left, right):
    return lax.dot_general(
        left, right, (((1,), (1,)), ((), ())), preferred_element_type=jnp.float32
    )


def shards(
    tokens,
    attn_gain,
    query_weight,
    key_cache,
    value_cache,
    head_lambda,
    head_gain,
    out_weight,
    mlp_gain,
    gate_weight,
    up_weight,
    down_weight,
):
    row_count = tokens.shape[0]
    kv_count = lax.axis_size("kv")
    tp_count = lax.axis_size("tp")
    kv_index = lax.axis_index("kv")
    row_span = query_weight.shape[0]
    full_rows = lax.all_gather(tokens, ("kv", "tp"), axis=1, tiled=True)
    wide_rows = full_rows.astype(jnp.float32)
    mean_square = jnp.mean(wide_rows * wide_rows, axis=-1, keepdims=True)
    scaled = (wide_rows * attn_gain).astype(jnp.bfloat16)
    local_cols = lax.dynamic_slice_in_dim(scaled, kv_index * row_span, row_span, 1)
    queries = lax.psum(jnp.dot(local_cols, query_weight, preferred_element_type=jnp.float32), "kv")
    queries = queries * lax.rsqrt(mean_square + EPS)
    head_count = head_lambda.shape[0]
    kv_local = key_cache.shape[2]
    group_size = head_count // kv_local
    position_count = key_cache.shape[1]
    half_dim = key_cache.shape[3] // 2
    value_dim = value_cache.shape[3]
    queries = queries.reshape(row_count, kv_local, group_size, 2, half_dim)
    rotated = rotate(queries, jnp.float32(position_count * kv_count)).astype(jnp.bfloat16)
    key_grid = key_cache.reshape(row_count, position_count, kv_local, 2, half_dim)
    scores = jnp.einsum(
        "bkgch,bpkch->bkgcp", rotated, key_grid, preferred_element_type=jnp.float32
    ) * half_dim ** (-0.5)
    local_peak = jnp.max(scores, axis=-1)
    weights_exp = jnp.exp(scores - local_peak[..., None])
    lam_grid = head_lambda.reshape(kv_local, group_size)[None, :, :, None]
    exp_total = jnp.sum(weights_exp, axis=-1)
    weighted = jnp.einsum(
        "bkgcp,bpkv->bkgcv",
        weights_exp.astype(jnp.bfloat16),
        value_cache,
        preferred_element_type=jnp.float32,
    )
    peak_all, total_all, weighted_all = merged((local_peak, exp_total, weighted), "kv", combine)
    attended = weighted_all / total_all[..., None]
    difference = attended[:, :, :, 0] - lam_grid * attended[:, :, :, 1]
    head_norm = lax.rsqrt(jnp.mean(difference * difference, axis=-1, keepdims=True) + EPS)
    head_out = (difference * head_norm * head_gain).reshape(row_count, head_count * value_dim)
    head_out = head_out.astype(jnp.bfloat16)
    out_part = inner_last(head_out, out_weight).astype(jnp.bfloat16)
    pieces = lax.all_gather(out_part, ("kv", "tp"), axis=1, tiled=True)
    attention = jnp.sum(
        pieces.astype(jnp.float32).reshape(row_count, kv_count, tp_count, -1), axis=2
    )
    stream = wide_rows + attention.reshape(row_count, -1)
    stream_square = jnp.mean(stream * stream, axis=-1, keepdims=True)
    normed = (stream * lax.rsqrt(stream_square + EPS) * mlp_gain).astype(jnp.bfloat16)
    gate_out = inner_last(normed, gate_weight)
    up_out = inner_last(normed, up_weight)
    hidden = (jax.nn.silu(gate_out) * up_out).astype(jnp.bfloat16)
    own_cols = tokens.shape[1]
    down_cols = lax.psum_scatter(
        lax.dot_general(
            down_weight, hidden, (((0,), (1,)), ((), ())), preferred_element_type=jnp.float32
        ),
        ("kv", "tp"),
        scatter_dimension=0,
        tiled=True,
    )
    column_index = lax.axis_index(("kv", "tp"))
    own_stream = lax.dynamic_slice_in_dim(stream, column_index * own_cols, own_cols, 1)
    return (own_stream + down_cols.T).astype(jnp.bfloat16)


def fused_kernel(
    kv_n, tp_n, tok_h, again_h, wq_h, kc_h, vc_h, lam_h, hgain_h, wo_h, mgain_h, wg_h, wu_h, wd_h,
    table_h,
    out,
    again, lam, hgain, mgain, table,
    wq, kc, vc, wo, wo_t, stage, wgu_t, wd,
    tg, qa, qf, ms, mv, st, cf, hf, oa, og, stream, ga, hid, ds, dr,
    hand, lsem, wsem, csem, sent, trecv, qrecv, srecv, mrecv, orecv, drecv,
):
    kv, tp = lax.axis_index("kv"), lax.axis_index("tp")
    n_all = kv_n * tp_n
    me = kv * tp_n + tp
    rows, own = tg.shape[1:]
    mate = {"kv": kv, "tp": lax.rem(tp + 1, tp_n)}
    heads, value_dim = qf.shape[0], qf.shape[2]
    group = heads // 2
    both = 2 * group
    features = wo.shape[0]
    units = wd.shape[0]
    per_weight = units // LANES
    chunks = 2 * per_weight
    slots = stage.shape[0]

    span = group * value_dim

    def query_load(side, g):
        at = pl.ds(pl.multiple_of(lax.rem(tp + side, tp_n) * own, LANES), own)
        cols = pl.ds(g * span, span)
        return pltpu.make_async_copy(
            wq_h.at[at, cols], wq.at[at, cols], wsem.at[side * 2 + g]
        )

    token_load = pltpu.make_async_copy(tok_h, tg.at[me], lsem.at[0])
    token_load.start()
    for side in range(2):
        for g in range(2):
            query_load(side, g).start()
    small_loads = [
        pltpu.make_async_copy(source, target, lsem.at[slot + 1])
        for slot, (source, target) in enumerate(
            [(again_h, again), (table_h, table), (lam_h, lam), (hgain_h, hgain), (mgain_h, mgain)]
        )
    ]
    for load in small_loads:
        load.start()

    down_rows = units // AHEAD
    marks = [chunks * mark // MARKS[-1] for mark in MARKS]

    def chunk_load(weight, i, slot):
        piece = pl.ds(pl.multiple_of(i * LANES, LANES), LANES)
        return pltpu.make_async_copy(weight.at[piece], stage.at[slot], csem.at[slot])

    def down_piece(i):
        piece = pl.ds(pl.multiple_of(i * down_rows, 8), down_rows)
        return pltpu.make_async_copy(wd_h.at[piece], wd.at[piece], wsem.at[3])

    def start_load(i):
        if isinstance(i, int):
            if i < per_weight:
                chunk_load(wg_h, i, i % slots).start()
            elif i < chunks:
                chunk_load(wu_h, i - per_weight, i % slots).start()
            else:
                down_piece(i - chunks).start()
            return

        @pl.when(i < per_weight)
        def _():
            chunk_load(wg_h, i, lax.rem(i, slots)).start()

        @pl.when((i >= per_weight) & (i < chunks))
        def _():
            chunk_load(wu_h, i - per_weight, lax.rem(i, slots)).start()

        @pl.when(i >= chunks)
        def _():
            down_piece(i - chunks).start()

    def loaded(which):
        for i in which:
            start_load(i + AHEAD)
        for i in which:
            slot = i % slots if isinstance(i, int) else lax.rem(i, slots)
            chunk_load(wg_h, 0, slot).wait()

    def transpose(which):
        for i in which:
            if isinstance(i, int):
                slot, weight, at = i % slots, i // per_weight, i % per_weight * LANES
            else:
                slot, weight = lax.rem(i, slots), lax.div(i, per_weight)
                at = pl.multiple_of(lax.rem(i, per_weight) * LANES, LANES)
            wgu_t[weight, :, pl.ds(at, LANES)] = stage[slot].T

    def turn(low, high):
        def pair(i, carry):
            which = (low + 2 * i, low + 2 * i + 1)
            loaded(which)
            transpose(which)
            return carry

        lax.fori_loop(0, (high - low) // 2, pair, 0)
        if (high - low) % 2:
            loaded((high - 1,))
            transpose((high - 1,))

    def turn_out():
        def pair(i, carry):
            for side in range(2):
                at = pl.ds(pl.multiple_of((2 * i + side) * LANES, LANES), LANES)
                wo_t[:, at] = wo[at, :].T
            return carry

        lax.fori_loop(0, features // LANES // 2, pair, 0)

    half_way = kv_n // 2

    def far(i):
        down = kv_n - 1 - i
        down = down - 1 + lax.div(down - kv + kv_n - 1, kv_n)
        up = i + 1 - lax.div(kv - i + kv_n - 1, kv_n)
        low = 1 - lax.div(kv, half_way)
        return up + low * (down - up)

    others = [far(i) for i in range(kv_n - 1)]

    def remote(ref, send, recv, where, target=None):
        pltpu.make_async_remote_copy(
            src_ref=ref, dst_ref=ref if target is None else target, send_sem=sent.at[send],
            recv_sem=recv, device_id=where, device_id_type=pl.DeviceIdType.MESH,
        ).start()

    def batch(ref, send, recv):
        return pltpu.make_async_remote_copy(
            src_ref=ref, dst_ref=ref, send_sem=send, recv_sem=recv,
            device_id=mate, device_id_type=pl.DeviceIdType.MESH,
        )

    def arrived(ref, recv):
        batch(ref, recv, recv).wait_recv()

    def signal(semaphore, where):
        pl.semaphore_signal(
            semaphore, inc=1, device_id=where, device_id_type=pl.DeviceIdType.MESH
        )

    barrier = pltpu.get_barrier_semaphore()
    for z in others:
        signal(barrier, {"kv": z, "tp": tp_n - 1})

    @pl.when(tp == tp_n - 1)
    def _():
        signal(barrier, mate)

    @pl.when(tp == 0)
    def _():
        pl.semaphore_wait(barrier, 1)
        signal(hand.at[0], mate)

    @pl.when(tp == tp_n - 1)
    def _():
        pl.semaphore_wait(hand.at[0], 1)

    token_load.wait()
    remote(tg.at[me], 0, trecv.at[0], mate)
    small_loads[0].wait()
    at_mate = kv * tp_n + lax.rem(tp + 1, tp_n)
    def scaled_half(side):
        at = kv * tp_n + lax.rem(tp + side, tp_n)
        gain = again[:, pl.ds(pl.multiple_of(at * own, LANES), own)]
        wide = tg[at].astype(jnp.float32)
        return (wide * gain).astype(jnp.bfloat16), jnp.sum(wide * wide, axis=1, keepdims=True)

    def half_product(scaled, side, g):
        query_load(side, g).wait()
        at = pl.ds(pl.multiple_of(lax.rem(tp + side, tp_n) * own, LANES), own)
        return jnp.dot(
            scaled, wq[at, g * span:(g + 1) * span], preferred_element_type=jnp.float32
        )

    def query_group(g):
        return pl.ds(g * (group + 1), group + 1 - g)

    scaled, own_square = scaled_half(0)
    partial = [half_product(scaled, 0, g) for g in range(2)]
    key_load = pltpu.make_async_copy(kc_h, kc, wsem.at[0])
    value_load = pltpu.make_async_copy(vc_h, vc, wsem.at[1])
    out_load = pltpu.make_async_copy(wo_h, wo, wsem.at[2])
    down_load = pltpu.make_async_copy(wd_h, wd, wsem.at[3])
    key_load.start()
    value_load.start()
    for i in range(AHEAD):
        start_load(i)
    arrived(tg.at[at_mate], trecv.at[0])
    scaled, square = scaled_half(1)
    qa[kv, 0] = jnp.broadcast_to(own_square + square, (rows, value_dim))


    def query_half(g):
        product = partial[g] + half_product(scaled, 1, g)
        for i in range(group):
            qa[kv, 1 + g * group + i] = product[:, i * value_dim:(i + 1) * value_dim]

    query_half(0)
    @pl.when(tp == tp_n - 1)
    def _():
        pl.semaphore_wait(barrier, tp_n * (kv_n - 1))
        signal(hand.at[1], mate)

    @pl.when(tp == 0)
    def _():
        pl.semaphore_wait(hand.at[1], 1)

    for g in range(2):
        if g:
            query_half(1)
        part = query_group(g)
        for z in others:
            remote(qa.at[kv, part], 1, qrecv.at[g], {"kv": z, "tp": tp})

    turn(marks[0], marks[1])
    out_load.start()
    turn(marks[1], marks[2])
    for load in small_loads[1:]:
        load.wait()
    lane = lax.broadcasted_iota(jnp.int32, (rows, value_dim), 1)
    half = value_dim // 2
    first = lax.rem(lane, half) < half // 2
    cosines = table[0:1, :]
    sines = table[1:2, :]
    low = lax.broadcasted_iota(jnp.int32, (group, value_dim), 1) < half
    row_at = lax.broadcasted_iota(jnp.int32, (both, value_dim), 0)
    lane_at = lax.broadcasted_iota(jnp.int32, (both, value_dim), 1)

    def rotate_group(g, scale):
        for h in range(g * group, (g + 1) * group):
            total = qa[0, 1 + h]
            for z in range(1, kv_n):
                total = total + qa[z, 1 + h]
            total = total * scale
            swapped = jnp.where(
                first,
                pltpu.roll(total, value_dim - half // 2, 1),
                pltpu.roll(total, half // 2, 1),
            )
            qf[h] = total * cosines + swapped * sines

    def attend_group(g, beside):
        transpose(beside)
        spread = []
        for b in range(rows):
            query = qf[g * group:(g + 1) * group, b, :]
            grid = jnp.concatenate(
                [jnp.where(low, query, 0.0), jnp.where(low, 0.0, query)], axis=0
            ).astype(jnp.bfloat16)
            scores = inner_last(grid, kc[b]) * half ** (-0.5)
            peak = jnp.max(scores, axis=1, keepdims=True)
            exps = jnp.exp(scores - peak)
            sums = jnp.sum(exps, axis=1, keepdims=True)
            spread.append(exps.astype(jnp.bfloat16))
            stats = jnp.where(lane_at == row_at, peak, 0.0) + jnp.where(
                lane_at == row_at + both, sums, 0.0
            )
            st[kv, g, b:b + 1, :] = jnp.sum(stats, axis=0, keepdims=True)
        for b in range(rows):
            values = jnp.dot(spread[b], vc[b], preferred_element_type=jnp.float32)
            ms[g, b] = values
            mv[kv, g, b] = values.astype(jnp.bfloat16)
        for z in others:
            remote(st.at[kv, g], 2, srecv.at[g], {"kv": z, "tp": tp})
            remote(mv.at[kv, g], 3, mrecv.at[g], {"kv": z, "tp": tp})

    rest = pl.ds(0, kv_n - 1)
    arrived(qa.at[rest, query_group(0)], qrecv.at[0])
    square = qa[0, 0]
    for z in range(1, kv_n):
        square = square + qa[z, 0]
    scale = lax.rsqrt(square / (n_all * own) + EPS)
    rotate_group(0, scale)
    key_load.wait()
    value_load.wait()
    loaded(range(marks[2], marks[3]))
    attend_group(0, range(marks[2], marks[3]))
    arrived(qa.at[rest, query_group(1)], qrecv.at[1])
    rotate_group(1, scale)
    loaded(range(marks[3], marks[4]))
    attend_group(1, range(marks[3], marks[4]))

    for z in others:
        for side in range(tp_n):
            remote(tg.at[me], 0, trecv.at[1], {"kv": z, "tp": side})
    turn(marks[4], marks[5])
    out_load.wait()
    turn_out()
    lam_at = lax.broadcasted_iota(jnp.int32, (heads, heads), 0)
    lam_lane = lax.broadcasted_iota(jnp.int32, (heads, heads), 1)
    lam_col = jnp.sum(
        jnp.where(lam_at == lam_lane, lam[...], 0.0), axis=1, keepdims=True
    )
    sources = [kv] + others[::-1]

    def factor_group(g):
        signs = jnp.concatenate(
            [jnp.ones((group, 1), jnp.float32), -lam_col[g * group:(g + 1) * group]], axis=0
        )
        for b in range(rows):
            peaks, sums = [], []
            for z in sources:
                stats = st[z, g, b:b + 1, :]
                peaks.append(
                    jnp.sum(jnp.where(lane_at == row_at, stats, 0.0), axis=1, keepdims=True)
                )
                sums.append(
                    jnp.sum(
                        jnp.where(lane_at == row_at + both, stats, 0.0), axis=1, keepdims=True
                    )
                )
            top = peaks[0]
            for peak in peaks[1:]:
                top = jnp.maximum(top, peak)
            factors = [jnp.exp(peak - top) for peak in peaks]
            all_sums = jnp.zeros_like(top)
            for factor, total in zip(factors, sums):
                all_sums = all_sums + total * factor
            share = signs / all_sums
            for at, factor in enumerate(factors):
                cf[at, b] = jnp.broadcast_to(factor * share, (both, value_dim))

    def merge_group(g):
        for b in range(rows):
            weighted = ms[g, b] * cf[0, b]
            for at, z in enumerate(sources[1:]):
                weighted = weighted + mv[z, g, b].astype(jnp.float32) * cf[at + 1, b]
            difference = weighted[0:group] + weighted[group:both]
            norm = lax.rsqrt(jnp.mean(difference * difference, axis=1, keepdims=True) + EPS)
            hf[b] = difference * norm * hgain[...]
        return jnp.concatenate(
            [hf[:, h, :] for h in range(group)], axis=1
        ).astype(jnp.bfloat16)

    cut = features // 2
    for g in range(2):
        arrived(st.at[rest, g], srecv.at[g])
        factor_group(g)
        arrived(mv.at[rest, g], mrecv.at[g])
        flat = merge_group(g)
        if g == 0:
            loaded(range(marks[5], marks[6]))
            transpose(range(marks[5], marks[6]))
            oa[...] = jnp.dot(flat, wo_t[0:span, :], preferred_element_type=jnp.float32)
    near = others[::-1]
    loaded(range(marks[6], marks[7]))
    transpose(range(marks[6], marks[7]))
    part = jnp.dot(flat, wo_t[span:2 * span, :], preferred_element_type=jnp.float32)
    og[me] = (oa[...] + part).astype(jnp.bfloat16)
    remote(og.at[me], 4, orecv.at[kv], mate)
    for z in near:
        for side in range(tp_n):
            remote(og.at[me], 4, orecv.at[kv], {"kv": z, "tp": side})

    turn(marks[7], marks[8])
    arrived(tg.at[pl.ds(0, n_all - tp_n)], trecv.at[1])
    square = jnp.zeros((rows, 1), jnp.float32)
    for order, z in enumerate(sources):
        if order == 0:
            arrived(og.at[at_mate], orecv.at[kv])
        else:
            arrived(og.at[pl.ds(z * tp_n, tp_n)], orecv.at[z])
        tokens = jnp.concatenate(
            [tg[z * tp_n + side].astype(jnp.float32) for side in range(tp_n)], axis=1
        )
        attention = og[z * tp_n].astype(jnp.float32)
        for side in range(1, tp_n):
            attention = attention + og[z * tp_n + side].astype(jnp.float32)
        piece = tokens + attention
        at = pl.ds(pl.multiple_of(z * features, LANES), features)
        stream[:, at] = piece
        square = square + jnp.sum(piece * piece, axis=1, keepdims=True)
        gained = (piece * mgain[:, at]).astype(jnp.bfloat16)
        for g in range(2):
            product = jnp.dot(gained, wgu_t[g, at, :], preferred_element_type=jnp.float32)
            if order == 0:
                ga[g] = product
            else:
                ga[g] = ga[g] + product
    scale = lax.rsqrt(square / (n_all * own) + EPS)
    gate = ga[0] * scale
    up = ga[1] * scale
    hid[...] = (gate / (1.0 + jnp.exp(-gate)) * up).astype(jnp.bfloat16)
    hidden = hid[...]
    down_load.wait()

    def down_block(at):
        return jnp.dot(
            hidden,
            wd[:, pl.ds(pl.multiple_of(at * own, LANES), own)],
            preferred_element_type=jnp.float32,
        )

    targets = []
    for z in others:
        for side in range(tp_n):
            targets.append((z * tp_n + side, {"kv": z, "tp": side}))
    targets.append((at_mate, mate))
    pending = None

    def down_send(slot, block):
        at, where = targets[slot]
        ds[at] = block.astype(ds.dtype)
        remote(ds.at[at], 5, drecv.at[0], where, dr.at[me])

    for slot, (at, _) in enumerate(targets):
        block = down_block(at)
        if pending is not None:
            down_send(slot - 1, pending)
        pending = block
    total = down_block(me)
    down_send(len(targets) - 1, pending)
    total = total + stream[:, pl.ds(pl.multiple_of(me * own, LANES), own)]
    arrived(dr.at[pl.ds(0, n_all - 1)], drecv.at[0])
    total = total + dr[at_mate].astype(jnp.float32)
    for z in others[::-1]:
        for side in range(tp_n):
            total = total + dr[z * tp_n + side].astype(jnp.float32)
    out[...] = total.astype(out.dtype)
    apart = pl.ds(0, n_all - 1)
    for slot, ref in enumerate(
        [tg.at[apart], qa.at[rest], st.at[rest], mv.at[rest], og.at[apart], ds.at[apart]]
    ):
        batch(ref, sent.at[slot], sent.at[slot]).wait_send()


def turning(head_dim, position):
    half_len = head_dim // 4
    inv_freq = np.float32(1.0) / np.float32(THETA) ** (
        np.arange(half_len, dtype=np.float32) / np.float32(half_len)
    )
    angles = (np.float32(position) * inv_freq.astype(np.float32)).astype(np.float32)
    cos, sin = np.cos(angles), np.sin(angles)
    return np.stack(
        [np.concatenate([cos, cos] * 2), np.concatenate([-sin, sin] * 2)]
    ).astype(np.float32)


def fused(kv_n, tp_n, *arrays):
    (tokens, attn_gain, wq, kc, vc, lam, hgain, wo, mgain, wg, wu, wd) = arrays
    rows, own = tokens.shape
    n_all = kv_n * tp_n
    positions, value_dim = kc.shape[1], kc.shape[3]
    heads = lam.shape[0]
    model = n_all * own
    per_weight = wg.shape[0] // LANES
    slots = AHEAD + 2
    f32, bf16 = jnp.float32, jnp.bfloat16
    table = jnp.asarray(turning(value_dim, positions * kv_n))
    dma = pltpu.SemaphoreType.DMA
    hbm = pl.BlockSpec(memory_space=pl.ANY)
    return pl.pallas_call(
        functools.partial(fused_kernel, kv_n, tp_n),
        out_shape=pltpu.VMEM((rows, own), tokens.dtype),
        in_specs=[hbm] * 13,
        out_specs=pl.BlockSpec(memory_space=pltpu.VMEM),
        scratch_shapes=[
            pltpu.VMEM((1, model), f32),
            pltpu.VMEM((1, heads), f32),
            pltpu.VMEM((1, value_dim), f32),
            pltpu.VMEM((1, model), f32),
            pltpu.VMEM((2, value_dim), f32),
            pltpu.VMEM(wq.shape, bf16),
            pltpu.VMEM((rows, positions, value_dim), bf16),
            pltpu.VMEM((rows, positions, value_dim), bf16),
            pltpu.VMEM(wo.shape, bf16),
            pltpu.VMEM(wo.shape[::-1], bf16),
            pltpu.VMEM((slots, LANES, model), bf16),
            pltpu.VMEM((2,) + wg.shape[::-1], bf16),
            pltpu.VMEM(wd.shape, bf16),
            pltpu.VMEM((n_all, rows, own), bf16),
            pltpu.VMEM((kv_n, heads + 1, rows, value_dim), f32),
            pltpu.VMEM((heads, rows, value_dim), f32),
            pltpu.VMEM((2, rows, heads, value_dim), f32),
            pltpu.VMEM((kv_n, 2, rows, heads, value_dim), bf16),
            pltpu.VMEM((kv_n, 2, rows, value_dim), f32),
            pltpu.VMEM((kv_n, rows, heads, value_dim), f32),
            pltpu.VMEM((rows, heads // 2, value_dim), f32),
            pltpu.VMEM((rows, wo.shape[0]), f32),
            pltpu.VMEM((n_all, rows, wo.shape[0]), bf16),
            pltpu.VMEM((rows, model), f32),
            pltpu.VMEM((2, rows, wg.shape[0]), f32),
            pltpu.VMEM((rows, wg.shape[0]), bf16),
            pltpu.VMEM((n_all, rows, own), bf16),
            pltpu.VMEM((n_all, rows, own), bf16),
            pltpu.SemaphoreType.REGULAR((2,)),
            dma((6,)), dma((4,)), dma((slots,)), dma((6,)),
            dma((2,)), dma((2,)), dma((2,)), dma((2,)), dma((kv_n,)), dma((1,)),
        ],
        compiler_params=pltpu.CompilerParams(
            collective_id=0, has_side_effects=True, vmem_limit_bytes=65000000
        ),
    )(
        tokens, attn_gain.reshape(1, -1), wq,
        kc.reshape(rows, positions, value_dim), vc.reshape(rows, positions, value_dim),
        lam.reshape(1, -1), hgain.reshape(1, -1), wo, mgain.reshape(1, -1), wg, wu, wd, table,
    )


def layer(kv_n, tp_n, *arrays):
    tokens, kc, lam, wo, wg = arrays[0], arrays[3], arrays[5], arrays[7], arrays[9]
    units = wg.shape[0]
    small = tokens.shape[0] == kv_n and kc.shape[2] == 1 and tp_n == 2 and kv_n % 2 == 0
    whole = tokens.shape[1] % LANES == 0 and wo.shape[0] % (2 * LANES) == 0
    whole = whole and kc.shape[3] == LANES and lam.shape[0] % 2 == 0
    if small and whole and units % LANES == 0 and units % (8 * AHEAD) == 0:
        return fused(kv_n, tp_n, *arrays)
    return shards(*arrays)


def solution(mesh):
    placed = (
        P("dp", ("kv", "tp")),
        P(),
        P("kv", "tp"),
        P("dp", "kv", "tp", None),
        P("dp", "kv", "tp", None),
        P("tp"),
        P(),
        P("kv", "tp"),
        P(),
        P(("kv", "tp"), None),
        P(("kv", "tp"), None),
        P(("kv", "tp"), None),
    )
    return jax.shard_map(
        functools.partial(layer, mesh.shape["kv"], mesh.shape["tp"]),
        mesh=mesh, in_specs=placed, out_specs=P("dp", ("kv", "tp")), check_vma=False
    )
```
